32 devices in a mesh: ep: 8 (over z, core), tp: 4 (over y, x).
Axes of the slice: x: 2, y: 2, z: 4, core: 2. Of those that a mesh axis runs over, the one named last changes fastest.
Arguments:
- tokens: bfloat16 [512, 4096], P('ep', 'tp'), may hold values from -600 to 600
- in_gain: float32 [4096], P('tp'), may hold values from 0.1 to 1.9
- out_gain: float32 [4096], P('tp'), may hold values from 0.1 to 1.9
- routes: int32 [512, 4], replicated, may hold values from 0 to 31, as said below
- route_weights: float32 [512, 4], replicated, may hold values from 0.05 to 1
- w_gate: bfloat16 [32, 4096, 1024], P('ep', 'tp'), may hold values from -0.09375 to 0.09375
- w_up: bfloat16 [32, 4096, 1024], P('ep', 'tp'), may hold values from -0.09375 to 0.09375
- w_down: bfloat16 [32, 1024, 4096], P('ep', None, 'tp'), may hold values from -0.375 to 0.375
Outputs:
- result: bfloat16 [512, 4096], P('ep', 'tp')
The draws below stay inside these ranges and needn't reach their ends.
Inputs may be any that keep to these rules, and one draw needn't show every extreme that they name: `routes`: each row names 4 different experts, all in one group of 8 consecutive numbers. In the rows of one index of ep (aligned blocks of 64 rows) no expert is named by more than 16 rows, and some expert by exactly 16.
All inputs are finite; a program needn't handle non-finite values.
Results may differ from the reference program's by a relative error of at most 0.025.
Values may be sent and summed in bfloat16 or wider, within the bound.
A program may use at most 64 MiB of HBM per device.

```python
import math
import jax
import jax.numpy as jnp
from jax import lax

D = 4096
FF = 1024
EXP_DEV = 4
GROUP_SIZE = 8
TOP = 4
TOK_DEV = 64
SPECIALIST_COUNT = 32
GROUPS = 4
TOKENS = 512
CAP = 16
N_EP = 8
N_TP = 4


def column_scale(key):
    columns = jnp.arange(D, dtype=jnp.float32) / D
    return jnp.exp(math.log(3.0) * columns + math.log(2.0) * jax.random.uniform(key, (D,), jnp.float32))


def draw_tokens(key, part):
    key_base, key_rows, key_cols = jax.random.split(jax.random.fold_in(key, 3), 3)
    base = jnp.clip(jax.random.normal(key_base, (TOKENS, D), jnp.float32), -6.0, 6.0)
    row_scale = jnp.exp(math.log(10.0) * jax.random.uniform(key_rows, (TOKENS, 1), jnp.float32))
    return (base * column_scale(key_cols) * row_scale).astype(jnp.bfloat16)


def draw_w_down(key, part):
    key_base, key_cols = jax.random.split(jax.random.fold_in(key, 5))
    base = jnp.clip(jax.random.normal(key_base, (SPECIALIST_COUNT, FF, D), jnp.float32), -6.0, 6.0)
    return (base * column_scale(key_cols) * FF ** (-0.5) / 3.0).astype(jnp.bfloat16)


def draw_routes(key, part):
    blocks = TOKENS // TOK_DEV
    key_rank, key_rows = jax.random.split(jax.random.fold_in(key, 7))
    ranking = jax.random.permutation(key_rank, SPECIALIST_COUNT).astype(jnp.int32)
    preferred_specialists = 12 * SPECIALIST_COUNT // (ranking + 1)
    numbers = jnp.arange(SPECIALIST_COUNT, dtype=jnp.int32)
    specialist_holders = numbers // EXP_DEV
    inside = jnp.arange(GROUP_SIZE, dtype=jnp.int32)
    group_ids = jnp.arange(GROUPS, dtype=jnp.int32)
    noise = jax.random.randint(key_rows, (blocks, TOK_DEV, SPECIALIST_COUNT), 0, 4 * SPECIALIST_COUNT, dtype=jnp.int32)

    def one_block(block, noise_rows):

        def step(counts, inputs):
            present_sequence_entry, jitter_for_entry = inputs
            destination_specialist = jnp.where(present_sequence_entry == 0, (block + blocks - 1) % blocks, (block + blocks // 2) % blocks)
            logit_offset = jnp.where((present_sequence_entry < 2) & (specialist_holders == destination_specialist), 64 * SPECIALIST_COUNT, 0).astype(jnp.int32)
            gating_logit = preferred_specialists + jitter_for_entry + logit_offset
            is_free = counts < CAP
            masked = jnp.where(is_free, gating_logit, -1).reshape(GROUPS, GROUP_SIZE)
            enough = jnp.sum(is_free.reshape(GROUPS, GROUP_SIZE).astype(jnp.int32), axis=1) >= TOP
            group_key = jnp.where(enough, jnp.max(masked, axis=1), -2) * GROUPS + group_ids
            chosen = jnp.argmax(group_key).astype(jnp.int32)
            within = lax.dynamic_index_in_dim(masked, chosen, 0, keepdims=False)
            best = lax.top_k(within * GROUP_SIZE + inside, TOP)[1].astype(jnp.int32)
            picked = chosen * GROUP_SIZE + best
            counts = counts + jnp.sum((picked[:, None] == numbers[None, :]).astype(jnp.int32), axis=0)
            return (counts, picked)
        row_ids = jnp.arange(TOK_DEV, dtype=jnp.int32)
        return lax.scan(step, jnp.zeros((SPECIALIST_COUNT,), jnp.int32), (row_ids, noise_rows))[1]
    picked_all = jax.vmap(one_block)(jnp.arange(blocks, dtype=jnp.int32), noise)
    return picked_all.reshape(TOKENS, TOP).astype(jnp.int32)


def block_scale(key, dims, cuts, smallest, top_value):
    factor_of, own = 1.0, jax.random.fold_in(key, 6)
    for dim, blocks in cuts:
        draws = jnp.exp(jax.random.uniform(jax.random.fold_in(own, dim), (blocks,), jnp.float32, smallest / len(cuts), top_value / len(cuts)))
        factor_of = factor_of * jnp.repeat(draws, dims[dim] // blocks).reshape([-1 if axis == dim else 1 for axis in range(len(dims))])
    return factor_of


def normal_values(stream_key, shape, width, limit, shards=(), kind=jnp.bfloat16):
    drawn = width * jax.random.normal(stream_key, shape, jnp.float32)
    if shards:
        drawn = drawn * block_scale(stream_key, shape, shards, -0.22, 0.18)
    return jnp.clip(drawn, -limit, limit).astype(kind)


def setup_inputs(seed: int = 0) -> dict:
    arg_keys = jax.random.split(jax.random.key(seed), 9)
    tokens = draw_tokens(jax.random.fold_in(arg_keys[8], 71), 0)
    in_gain = jnp.clip(1.0 + 0.18 * jax.random.normal(arg_keys[1], (D,), jnp.float32), 0.1, 1.9)
    out_gain = jnp.clip(1.0 + 0.18 * jax.random.normal(arg_keys[2], (D,), jnp.float32), 0.1, 1.9)
    routes = draw_routes(jax.random.fold_in(arg_keys[8], 71), 0)
    route_weights = jnp.clip(jax.random.uniform(arg_keys[4], (TOKENS, TOP), jnp.float32, 0.05, 1.0), 0.05, 1.0)
    w_gate = normal_values(arg_keys[5], (SPECIALIST_COUNT, D, FF), D ** -0.5, 0.09375, ((0, 8), (1, 4)))
    w_up = normal_values(arg_keys[6], (SPECIALIST_COUNT, D, FF), D ** -0.5, 0.09375, ((0, 8), (1, 4)))
    w_down = draw_w_down(jax.random.fold_in(arg_keys[8], 71), 0)
    return dict(tokens=tokens, in_gain=in_gain, out_gain=out_gain, routes=routes, route_weights=route_weights, w_gate=w_gate, w_up=w_up, w_down=w_down)


EPS = 1e-06

def reference(tokens, in_gain, out_gain, routes, route_weights, w_gate, w_up, w_down):
    values = tokens.astype(jnp.float32)
    normed = (values * lax.rsqrt(lax.optimization_barrier(jnp.mean(values * values, axis=1, keepdims=True)) + EPS) * in_gain).astype(jnp.bfloat16)
    local_width = D // N_TP
    slot_limit = N_EP * CAP

    def block_sum(slot_rows, weights):
        stacked = weights.astype(jnp.float32).reshape(N_TP, local_width, FF)
        parts = jnp.einsum('rjd,jdf->jrf', slot_rows, stacked).astype(jnp.bfloat16)
        parts = lax.optimization_barrier(parts)
        return lax.optimization_barrier(jnp.sum(parts.astype(jnp.float32), axis=0))

    def one_expert(combined, expert):
        matches = routes == expert
        weight = lax.optimization_barrier(jnp.sum(jnp.where(matches, route_weights, 0.0), axis=1))
        chosen = jnp.any(matches, axis=1)
        picked = jnp.nonzero(chosen, size=slot_limit, fill_value=0)[0].astype(jnp.int32)
        is_live = jnp.arange(slot_limit, dtype=jnp.int32) < jnp.sum(chosen.astype(jnp.int32))
        slot_rows = normed[picked].astype(jnp.float32).reshape(slot_limit, N_TP, local_width)
        gate_sum = block_sum(slot_rows, w_gate[expert])
        up_sum = block_sum(slot_rows, w_up[expert])
        active = (jax.nn.silu(gate_sum) * up_sum).astype(jnp.bfloat16)
        results = jnp.dot(active, w_down[expert], preferred_element_type=jnp.float32).astype(jnp.bfloat16)
        scale = jnp.where(is_live, weight[picked], 0.0)
        combined = combined.at[picked].add(scale[:, None] * results.astype(jnp.float32))
        return (combined, None)
    start = jnp.zeros((TOKENS, D), jnp.float32)
    combined, unused = lax.scan(one_expert, start, jnp.arange(SPECIALIST_COUNT, dtype=jnp.int32))
    squares = lax.optimization_barrier(jnp.mean(combined * combined, axis=1, keepdims=True))
    return (combined * lax.rsqrt(squares + EPS) * out_gain).astype(jnp.bfloat16)
```

```python
import functools

import jax
import jax.numpy as jnp
from jax import lax
from jax.experimental import pallas as pl
from jax.experimental.pallas import tpu as pltpu
from jax.sharding import PartitionSpec as P

D = 4096
GROUP = 8

EPS = 1e-06
MESH = pl.DeviceIdType.MESH
F32, BF16 = jnp.float32, jnp.bfloat16

ORDER = (
    "A0", "N1", "A1", "B0", "N2", "A2", "B1", "C0", "N3",
    "A3", "B2", "D0", "C1", "B3", "E0", "D1", "C2", "F0",
    "E1", "D2", "C3", "F1", "E2", "D3", "F2", "E3", "F3",
)


def iota(shape, dim):
    return lax.broadcasted_iota(jnp.int32, shape, dim)


def tdot(a, b):
    return lax.dot_general(a, b, (((0,), (0,)), ((), ())), preferred_element_type=F32)


def kernel(
    cfg,
    tokens_ref,
    in_gain_ref,
    out_gain_ref,
    routes_ref,
    weights_ref,
    wg_hbm,
    wu_hbm,
    wd_hbm,
    out_ref,
    wg,
    wu,
    wd,
    pick,
    slot_w,
    own_pick,
    send_rows,
    compact,
    rows,
    ss_out,
    ss_in,
    part,
    s1_in,
    s2_out,
    s2_in,
    act,
    res,
    comb,
    x_out,
    x_in,
    r_out,
    r_in,
    so_out,
    so_in,
    w_sem,
    d_send,
    d_recv,
    f_send,
    ss_send,
    ss_recv,
    s1_send,
    s1_recv,
    s2_send,
    s2_recv,
    g_send,
    g_recv,
    x_send,
    x_recv,
    r_send,
    r_recv,
    so_send,
    so_recv,
):
    n_z, tok, n_exp, cap, width, ff, top = cfg
    rows_z = cap * GROUP // top
    half = ff // 2
    slots = 2 * cap
    me = lax.axis_index("ep")
    tp = lax.axis_index("tp")
    z, core = me // 2, lax.rem(me, 2)
    other = 1 - core
    y, x = tp // 2, lax.rem(tp, 2)
    x_tp = 2 * y + (1 - x)
    y_tp = 2 * (1 - y) + x
    xy_tp = 2 * (1 - y) + (1 - x)
    partner = 2 * z + other
    peers = (x_tp, y_tp, xy_tp)

    def expert(p):
        return 2 * lax.rem(y + 1 - p % 2, 2) + lax.rem(x + 1 - p // 2, 2)

    def chip(c):
        return 2 * ((z // 2 + c // 2) % 2) + (z % 2 + c % 2) % 2

    def w_copy(k, p):
        hbm, vmem = ((wg_hbm, wg), (wu_hbm, wu), (wd_hbm, wd))[k]
        e = expert(p)
        return pltpu.make_async_copy(hbm.at[e], vmem.at[e], w_sem.at[k, p])

    for p in range(n_exp):
        w_copy(0, p).start()
        w_copy(1, p).start()
    for p in reversed(range(n_exp)):
        w_copy(2, p).start()

    barrier = pltpu.get_barrier_semaphore()
    for c in range(1, n_z):
        pl.semaphore_signal(
            barrier, inc=1, device_id={"ep": 2 * chip(c) + core}, device_id_type=MESH
        )
    for peer in peers:
        pl.semaphore_signal(barrier, inc=1, device_id={"tp": peer}, device_id_type=MESH)
    pl.semaphore_signal(barrier, inc=1, device_id={"ep": partner}, device_id_type=MESH)

    def remote(src, dst, send, recv, **dev):
        return pltpu.make_async_remote_copy(
            src_ref=src,
            dst_ref=dst,
            send_sem=send,
            recv_sem=recv,
            device_id=dev,
            device_id_type=MESH,
        )

    lane = iota((tok, n_z * rows_z), 1)
    group = routes_ref[pl.ds(me * tok, tok), :][:, 0:1] // GROUP
    hit = group == chip(lane // rows_z)
    before = (iota((tok, tok), 1) < iota((tok, tok), 0)).astype(BF16)
    rank = jnp.dot(before, jnp.where(hit, 1.0, 0.0).astype(BF16), preferred_element_type=F32)
    own = jnp.where(hit & (rank.astype(jnp.int32) == lane % rows_z), 1.0, 0.0).astype(BF16)
    own_pick[...] = own
    send_rows[...] = (
        tdot(own, tokens_ref[...]).astype(BF16).reshape(n_z, rows_z, width)
    )

    chunk_tok = 2 * tok
    n_slot = n_exp * slots
    s_lane = iota((chunk_tok, n_slot), 1)
    s_block = iota((chunk_tok, n_slot), 0) // tok
    r_lane = iota((chunk_tok, 2 * rows_z), 1)
    r_block = iota((chunk_tok, 2 * rows_z), 0) // tok

    def make_pick(c):
        first = chip(c) * chunk_tok
        routes = routes_ref[pl.ds(first, chunk_tok), :]
        weights = weights_ref[pl.ds(first, chunk_tok), :]
        t_row, t_col = iota((chunk_tok, chunk_tok), 0), iota((chunk_tok, chunk_tok), 1)
        earlier = jnp.where((t_col < t_row) & (t_col // tok == t_row // tok), 1.0, 0.0).astype(BF16)
        wanted = me * n_exp + s_lane // slots
        hits = jnp.zeros((chunk_tok, n_slot), F32)
        wt = jnp.zeros((chunk_tok, n_slot), F32)
        for k in range(top):
            match = routes[:, k : k + 1] == wanted
            hits = jnp.where(match, 1.0, hits)
            wt = jnp.where(match, weights[:, k : k + 1], wt)
        rank = jnp.dot(earlier, hits.astype(BF16), preferred_element_type=F32).astype(jnp.int32)
        in_slot = (
            (hits > 0.0) & (rank == s_lane % cap) & (s_block == s_lane // cap % 2)
        )
        grouped = (routes[:, 0:1] // GROUP == z) & (r_lane >= 0)
        g_rank = jnp.dot(
            earlier, jnp.where(grouped, 1.0, 0.0).astype(BF16), preferred_element_type=F32
        ).astype(jnp.int32)
        in_row = grouped & (g_rank == r_lane % rows_z) & (r_block == r_lane // rows_z)
        pick[c] = tdot(
            jnp.where(in_slot, 1.0, 0.0).astype(BF16), jnp.where(in_row, 1.0, 0.0).astype(BF16)
        ).astype(BF16).reshape(n_exp, slots, 2 * rows_z)
        wrow = jnp.sum(jnp.where(in_slot, wt, 0.0), axis=0, keepdims=True)
        mine = iota((slots, n_slot), 1) == tp * slots + iota((slots, n_slot), 0)
        wcol = jnp.sum(jnp.where(mine, wrow, 0.0), axis=1, keepdims=True)
        slot_w[c] = jnp.broadcast_to(wcol, (slots, 128))

    make_pick(0)
    pl.semaphore_wait(barrier, 4 + n_z - 1)

    def dispatch(c):
        return remote(
            send_rows.at[c], compact.at[c, core], d_send.at[c], d_recv.at[c, core],
            ep=2 * chip(c) + core,
        )

    def forward(c, block):
        src = send_rows.at[0] if c == 0 else compact.at[c, block]
        return remote(
            src, compact.at[c, block], f_send.at[c], d_recv.at[c, block], ep=partner
        )

    forward(0, core).start()
    for c in range(1, n_z):
        dispatch(c).start()
    compact[0, core] = send_rows[0]
    for c in range(1, n_z):
        make_pick(c)

    def square_copy(c, k):
        return remote(
            ss_out.at[c], ss_in.at[c, k], ss_send.at[c, k], ss_recv.at[c, k], tp=peers[k]
        )

    def s1(c, h, k, e):
        return remote(
            part.at[c, h, e], s1_in.at[c, h, k], s1_send.at[c, h, k], s1_recv.at[c, h, k],
            tp=peers[h],
        )

    def s2(c, h):
        return remote(
            s2_out.at[c, h], s2_in.at[c, h], s2_send.at[c, h], s2_recv.at[c, h], tp=peers[1 - h]
        )

    def gather(c, h, k):
        piece = act.at[c, h, tp]
        return remote(piece, piece, g_send.at[c, h, k], g_recv.at[c, h, k], tp=peers[k])

    def relay(c, h):
        piece = act.at[c, h, peers[h]]
        return remote(piece, piece, g_send.at[c, h, 2], g_recv.at[c, h, 2], tp=peers[1 - h])

    def swap(c):
        return remote(x_out.at[c], x_in.at[c], x_send.at[c], x_recv.at[c], ep=partner)

    def home(c):
        return remote(
            r_out.at[c], r_in.at[c], r_send.at[c], r_recv.at[c], ep=2 * chip(c) + core
        )

    def home_square(c, k):
        return remote(
            so_out.at[c], so_in.at[c, k], so_send.at[c, k], so_recv.at[c, k],
            ep=2 * chip(c) + core, tp=(x_tp, y_tp, xy_tp, tp)[k],
        )

    def take_in(c):
        dispatch(c).wait_recv()
        forward(c, core).start()

    def gate_up(c):
        forward(c, other).wait_recv()
        raw = compact[c].reshape(2 * rows_z, width).astype(F32)
        square = jnp.sum(raw * raw, axis=1, keepdims=True)
        diag = iota((2 * rows_z, 128), 0) == iota((2 * rows_z, 128), 1)
        row = jnp.sum(jnp.where(diag, square, 0.0), axis=0, keepdims=True)
        ss_out[c] = jnp.broadcast_to(row, (8, 128))
        for k in range(3):
            square_copy(c, k).start()
        gained = (raw * in_gain_ref[...]).astype(BF16)
        rows[...] = (
            jnp.dot(pick[c].reshape(n_slot, 2 * rows_z), gained, preferred_element_type=F32)
            .astype(BF16)
            .reshape(n_exp, slots, width)
        )

        @pl.loop(0, n_exp)
        def _(p):
            e = expert(p)
            if c == 0:
                w_copy(0, p).wait()
                w_copy(1, p).wait()
            for h in range(2):
                cols = slice(h * half, (h + 1) * half)
                part[c, h, e, :, 0:half] = jnp.dot(
                    rows[e], wg[e, :, cols], preferred_element_type=F32
                ).astype(BF16)
                part[c, h, e, :, half:ff] = jnp.dot(
                    rows[e], wu[e, :, cols], preferred_element_type=F32
                ).astype(BF16)

                if h == 0:

                    @pl.when(p < 2)
                    def _():
                        s1(c, 0, p, e).start()

                else:

                    @pl.when(p % 2 == 0)
                    def _():
                        s1(c, 1, p // 2, e).start()

    def reduce_first(c):
        for h in range(2):
            e = peers[1 - h]
            s1(c, h, 0, e).wait_recv()
            s2_out[c, h] = (part[c, h, e].astype(F32) + s1_in[c, h, 0].astype(F32)).astype(BF16)
            s2(c, h).start()

    def activate(c):
        for k in range(3):
            square_copy(c, k).wait_recv()
        square = ss_out[c] + ss_in[c, 0] + ss_in[c, 1] + ss_in[c, 2]
        scale_row = lax.rsqrt(square[0:1, 0 : 2 * rows_z] / D + EPS)
        scale = jnp.sum(pick[c, tp].astype(F32) * scale_row, axis=1, keepdims=True)
        weight = slot_w[c][:, 0:1]
        for h in range(2):
            s1(c, h, 1, tp).wait_recv()
            s2(c, h).wait_recv()
            total = (
                part[c, h, tp].astype(F32)
                + s1_in[c, h, 1].astype(F32)
                + s2_in[c, h].astype(F32)
            ) * scale
            gate, up = total[:, 0:half], total[:, half:ff]
            act[c, h, tp] = (gate / (1.0 + jnp.exp(-gate)) * up * weight).astype(BF16)
            gather(c, h, h).start()
        gather(c, 1, 0).start()
        gather(c, 0, 1).start()

    def pass_on(c):
        for h in range(2):
            gather(c, h, h).wait_recv()
            relay(c, h).start()

    def down(c):
        @pl.loop(0, n_exp)
        def _(i):
            p = n_exp - 1 - i
            e = expert(p)

            @pl.when(i == 1)
            def _():
                gather(c, 0, 1).wait_recv()

            @pl.when(i == 2)
            def _():
                gather(c, 1, 0).wait_recv()

            @pl.when(i == 3)
            def _():
                for h in range(2):
                    relay(c, h).wait_recv()

            if c == 0:
                w_copy(2, p).wait()
            res[e] = (
                jnp.dot(act[c, 0, e], wd[e, 0:half, :], preferred_element_type=F32)
                + jnp.dot(act[c, 1, e], wd[e, half:ff, :], preferred_element_type=F32)
            ).astype(BF16)

        comb[c] = tdot(
            pick[c].reshape(n_slot, 2 * rows_z), res[...].reshape(n_slot, width)
        ).reshape(2, rows_z, width)
        x_out[c] = comb[c, other].astype(BF16)
        swap(c).start()

    def send_home(c):
        swap(c).wait_recv()
        total = comb[c, core] + x_in[c].astype(F32)
        square = jnp.sum(total * total, axis=1, keepdims=True)
        diag = c * rows_z + iota((rows_z, 128), 0) == iota((rows_z, 128), 1)
        row = jnp.sum(jnp.where(diag, square, 0.0), axis=0, keepdims=True)
        so_out[c] = jnp.broadcast_to(row, (8, 128))
        if c:
            r_out[c] = total.astype(BF16)
            home(c).start()
        else:
            r_in[0] = total.astype(BF16)
            so_in[0, 3] = so_out[0]
        for k in range(4 if c else 3):
            home_square(c, k).start()

    stage = {
        "A": gate_up,
        "B": reduce_first,
        "C": activate,
        "D": pass_on,
        "E": down,
        "F": send_home,
        "N": take_in,
    }
    for step in ORDER:
        stage[step[0]](int(step[1]))

    square = so_in[0, 3]
    for c in range(n_z):
        if c:
            home(c).wait_recv()
        for k in range(4 if c else 3):
            home_square(c, k).wait_recv()
            square = square + so_in[c, k]
    combined = jnp.dot(
        own_pick[...], r_in[...].reshape(n_z * rows_z, width), preferred_element_type=F32
    )
    scale_row = lax.rsqrt(square[0:1, :] / D + EPS)
    scale = jnp.sum(own_pick[...].astype(F32) * scale_row, axis=1, keepdims=True)
    out_ref[...] = (combined * scale * out_gain_ref[...]).astype(BF16)

    for c in range(n_z):
        forward(c, core).wait_send()
        if c:
            dispatch(c).wait_send()
            home(c).wait_send()
        for k in range(3):
            square_copy(c, k).wait_send()
        for h in range(2):
            s1(c, h, 0, xy_tp).wait_send()
            s1(c, h, 1, peers[h]).wait_send()
            s2(c, h).wait_send()
            gather(c, h, 0).wait_send()
            gather(c, h, 1).wait_send()
            relay(c, h).wait_send()
        swap(c).wait_send()
        for k in range(4 if c else 3):
            home_square(c, k).wait_send()


def fused(mesh, tokens, in_gain, out_gain, routes, route_weights, w_gate, w_up, w_down):
    tok, width = tokens.shape
    top = routes.shape[1]
    n_exp, _, ff = w_gate.shape
    n_ep = mesh.shape["ep"]
    n_z = n_ep // 2
    cap = max(2, 2 * tok * top // (n_exp * n_ep))
    rows_z = cap * GROUP // top
    slots = 2 * cap
    cfg = (n_z, tok, n_exp, cap, width, ff, top)
    vmem = pl.BlockSpec(memory_space=pltpu.VMEM)
    hbm = pl.BlockSpec(memory_space=pl.ANY)
    dma = pltpu.SemaphoreType.DMA
    return pl.pallas_call(
        functools.partial(kernel, cfg),
        out_shape=jax.ShapeDtypeStruct((tok, width), BF16),
        in_specs=[vmem] * 5 + [hbm] * 3,
        out_specs=vmem,
        scratch_shapes=[
            pltpu.VMEM(w_gate.shape, BF16),
            pltpu.VMEM(w_up.shape, BF16),
            pltpu.VMEM(w_down.shape, BF16),
            pltpu.VMEM((n_z, n_exp, slots, 2 * rows_z), BF16),
            pltpu.VMEM((n_z, slots, 128), F32),
            pltpu.VMEM((tok, n_z * rows_z), BF16),
            pltpu.VMEM((n_z, rows_z, width), BF16),
            pltpu.VMEM((n_z, 2, rows_z, width), BF16),
            pltpu.VMEM((n_exp, slots, width), BF16),
            pltpu.VMEM((n_z, 8, 128), F32),
            pltpu.VMEM((n_z, 3, 8, 128), F32),
            pltpu.VMEM((n_z, 2, n_exp, slots, ff), BF16),
            pltpu.VMEM((n_z, 2, 2, slots, ff), BF16),
            pltpu.VMEM((n_z, 2, slots, ff), BF16),
            pltpu.VMEM((n_z, 2, slots, ff), BF16),
            pltpu.VMEM((n_z, 2, n_exp, slots, ff // 2), BF16),
            pltpu.VMEM((n_exp, slots, width), BF16),
            pltpu.VMEM((n_z, 2, rows_z, width), F32),
            pltpu.VMEM((n_z, rows_z, width), BF16),
            pltpu.VMEM((n_z, rows_z, width), BF16),
            pltpu.VMEM((n_z, rows_z, width), BF16),
            pltpu.VMEM((n_z, rows_z, width), BF16),
            pltpu.VMEM((n_z, 8, 128), F32),
            pltpu.VMEM((n_z, 4, 8, 128), F32),
            dma((3, n_exp)),
            dma((n_z,)),
            dma((n_z, 2)),
            dma((n_z,)),
            dma((n_z, 3)),
            dma((n_z, 3)),
            dma((n_z, 2, 2)),
            dma((n_z, 2, 2)),
            dma((n_z, 2)),
            dma((n_z, 2)),
            dma((n_z, 2, 3)),
            dma((n_z, 2, 3)),
            dma((n_z,)),
            dma((n_z,)),
            dma((n_z,)),
            dma((n_z,)),
            dma((n_z, 4)),
            dma((n_z, 4)),
        ],
        compiler_params=pltpu.CompilerParams(
            collective_id=0, has_side_effects=True, vmem_limit_bytes=60 * 2**20
        ),
    )(
        tokens,
        in_gain.reshape(1, width),
        out_gain.reshape(1, width),
        routes,
        route_weights,
        w_gate,
        w_up,
        w_down,
    )


def run_experts(slot_rows, w_gate, w_up, w_down):
    gate_part = jnp.einsum(
        "secd,edf->secf", slot_rows, w_gate, preferred_element_type=jnp.float32
    ).astype(jnp.bfloat16)
    up_part = jnp.einsum(
        "secd,edf->secf", slot_rows, w_up, preferred_element_type=jnp.float32
    ).astype(jnp.bfloat16)
    gate_sum, up_sum = (
        lax.psum(gate_part, "tp").astype(jnp.float32),
        lax.psum(up_part, "tp").astype(jnp.float32),
    )
    active = (jax.nn.silu(gate_sum) * up_sum).astype(jnp.bfloat16)
    return jnp.einsum("secf,efd->secd", active, w_down, preferred_element_type=jnp.float32).astype(
        jnp.bfloat16
    )


def on_device(tokens, in_gain, out_gain, routes, route_weights, w_gate, w_up, w_down):
    tok_rows, local_width = tokens.shape
    top_count = routes.shape[1]
    local_experts = w_gate.shape[0]
    groups_ep = lax.axis_size("ep")
    experts = local_experts * groups_ep
    capacity = max(2, 2 * tok_rows * top_count // experts)
    values = tokens.astype(jnp.float32)
    sum_squares = lax.psum(jnp.sum(values * values, axis=1), "tp")
    normed = (values * lax.rsqrt(sum_squares / D + EPS)[:, None] * in_gain).astype(jnp.bfloat16)
    row_start = lax.axis_index("ep") * tok_rows
    my_routes = lax.dynamic_slice_in_dim(routes, row_start, tok_rows, 0)
    my_weights = lax.dynamic_slice_in_dim(route_weights, row_start, tok_rows, 0)
    flat_ids = my_routes.reshape(-1)
    matches = (flat_ids[:, None] == jnp.arange(experts, dtype=jnp.int32)[None, :]).astype(jnp.int32)
    slot_rank = jnp.sum((jnp.cumsum(matches, axis=0) - matches) * matches, axis=1)
    position = flat_ids * capacity + slot_rank
    dispatch_table = jnp.any(
        position.reshape(tok_rows, top_count, 1)
        == jnp.arange(experts * capacity, dtype=jnp.int32)[None, None, :],
        axis=1,
    )
    outgoing = jnp.einsum(
        "ts,td->sd", dispatch_table.astype(jnp.bfloat16), normed, preferred_element_type=jnp.float32
    ).astype(jnp.bfloat16)
    outgoing = outgoing.reshape(groups_ep, local_experts, capacity, local_width)
    answers = run_experts(
        lax.all_to_all(outgoing, "ep", split_axis=0, concat_axis=0, tiled=True),
        w_gate,
        w_up,
        w_down,
    )
    returned = lax.all_to_all(answers, "ep", split_axis=0, concat_axis=0, tiled=True)
    flat_out = returned.reshape(experts * capacity, local_width)
    picked = flat_out[position].reshape(tok_rows, top_count, local_width)
    combined = jnp.sum(my_weights[:, :, None] * picked.astype(jnp.float32), axis=1)
    out_squares = lax.psum(jnp.sum(combined * combined, axis=1), "tp")
    return (combined * lax.rsqrt(out_squares / D + EPS)[:, None] * out_gain).astype(jnp.bfloat16)


def solution(mesh):
    placed = (
        P("ep", "tp"),
        P("tp"),
        P("tp"),
        P(),
        P(),
        P("ep", "tp", None),
        P("ep", "tp", None),
        P("ep", None, "tp"),
    )
    body = on_device
    if mesh.shape["tp"] == 4 and mesh.shape["ep"] == 8:
        body = functools.partial(fused, mesh)
    return jax.shard_map(
        body, mesh=mesh, in_specs=placed, out_specs=P("ep", "tp"), check_vma=False
    )
```

```python
import functools

import jax
import jax.numpy as jnp
from jax import lax
from jax.experimental import pallas as pl
from jax.experimental.pallas import tpu as pltpu
from jax.sharding import PartitionSpec as P

D = 4096
GROUP = 8

EPS = 1e-06
MESH = pl.DeviceIdType.MESH
F32, BF16 = jnp.float32, jnp.bfloat16

ORDER = (
    "A0", "P1", "A1", "B0", "P2", "A2", "B1", "C0", "P3",
    "A3", "B2", "D0", "C1", "B3", "E0", "D1", "C2", "F0",
    "E1", "D2", "C3", "F1", "E2", "D3", "F2", "E3", "F3",
)


def iota(shape, dim):
    return lax.broadcasted_iota(jnp.int32, shape, dim)


def tdot(a, b):
    return lax.dot_general(a, b, (((0,), (0,)), ((), ())), preferred_element_type=F32)


def kernel(
    cfg,
    tokens_ref,
    in_gain_ref,
    out_gain_ref,
    routes_ref,
    weights_ref,
    wg_hbm,
    wu_hbm,
    wd_hbm,
    out_ref,
    wg,
    wu,
    wd,
    pick,
    slot_w,
    own_pick,
    send_rows,
    compact,
    rows,
    ss_out,
    ss_in,
    part,
    s1_in,
    s2_out,
    s2_in,
    act,
    res,
    comb,
    x_out,
    x_in,
    r_out,
    r_in,
    so_out,
    so_in,
    w_sem,
    d_send,
    d_recv,
    f_send,
    ss_send,
    ss_recv,
    s1_send,
    s1_recv,
    s2_send,
    s2_recv,
    g_send,
    g_recv,
    x_send,
    x_recv,
    r_send,
    r_recv,
    so_send,
    so_recv,
):
    n_z, tok, n_exp, cap, width, ff, top = cfg
    rows_z = cap * GROUP // top
    half = ff // 2
    slots = 2 * cap
    me = lax.axis_index("ep")
    tp = lax.axis_index("tp")
    z, core = me // 2, lax.rem(me, 2)
    other = 1 - core
    y, x = tp // 2, lax.rem(tp, 2)
    x_tp = 2 * y + (1 - x)
    y_tp = 2 * (1 - y) + x
    xy_tp = 2 * (1 - y) + (1 - x)
    partner = 2 * z + other
    peers = (x_tp, y_tp, xy_tp)

    def expert(p):
        return 2 * lax.rem(y + 1 - p % 2, 2) + lax.rem(x + 1 - p // 2, 2)

    def chip(c):
        return 2 * ((z // 2 + c // 2) % 2) + (z % 2 + c % 2) % 2

    def w_copy(k, p):
        hbm, vmem = ((wg_hbm, wg), (wu_hbm, wu), (wd_hbm, wd))[k]
        e = expert(p)
        return pltpu.make_async_copy(hbm.at[e], vmem.at[e], w_sem.at[k, p])

    for p in range(n_exp):
        w_copy(0, p).start()
        w_copy(1, p).start()
    for p in reversed(range(n_exp)):
        w_copy(2, p).start()

    barrier = pltpu.get_barrier_semaphore()
    for c in range(1, n_z):
        pl.semaphore_signal(
            barrier, inc=1, device_id={"ep": 2 * chip(c) + core}, device_id_type=MESH
        )
    for peer in peers:
        pl.semaphore_signal(barrier, inc=1, device_id={"tp": peer}, device_id_type=MESH)
    pl.semaphore_signal(barrier, inc=1, device_id={"ep": partner}, device_id_type=MESH)

    def remote(src, dst, send, recv, **dev):
        return pltpu.make_async_remote_copy(
            src_ref=src,
            dst_ref=dst,
            send_sem=send,
            recv_sem=recv,
            device_id=dev,
            device_id_type=MESH,
        )

    chunk_tok = 2 * tok
    n_slot = n_exp * slots
    n_row = n_z * rows_z

    def nt_dot(a, b):
        return lax.dot_general(a, b, (((1,), (1,)), ((), ())), preferred_element_type=F32)

    def chip_tokens(ref, c):
        return ref[:, pl.ds(pl.multiple_of(chip(c) * chunk_tok, chunk_tok), chunk_tok)]

    both = chip_tokens(routes_ref, 0)[0:1, :]
    group = jnp.where(core == 0, both[:, 0:tok], both[:, tok:chunk_tok]) // GROUP
    row_of = iota((n_row, tok), 0)
    hit = group == chip(row_of // rows_z)
    earlier = jnp.where(iota((tok, tok), 0) < iota((tok, tok), 1), 1.0, 0.0).astype(BF16)
    rank = jnp.dot(
        jnp.where(hit, 1.0, 0.0).astype(BF16), earlier, preferred_element_type=F32
    ).astype(jnp.int32)
    own = jnp.where(hit & (rank == row_of % rows_z), 1.0, 0.0)
    send_rows[...] = (
        jnp.dot(own.astype(BF16), tokens_ref[...], preferred_element_type=F32)
        .astype(BF16)
        .reshape(n_z, rows_z, width)
    )
    own_pick[...] = own.T.astype(BF16)

    def make_pick(c):
        routes = chip_tokens(routes_ref, c)
        weights = chip_tokens(weights_ref, c)
        t_row, t_col = iota((chunk_tok, chunk_tok), 0), iota((chunk_tok, chunk_tok), 1)
        earlier = jnp.where((t_row < t_col) & (t_col // tok == t_row // tok), 1.0, 0.0).astype(BF16)
        slot = iota((n_slot, chunk_tok), 0)
        slot_block = iota((n_slot, chunk_tok), 1) // tok
        wanted = me * n_exp + slot // slots
        hits = jnp.zeros((n_slot, chunk_tok), F32)
        wt = jnp.zeros((n_slot, chunk_tok), F32)
        for k in range(top):
            match = routes[k : k + 1, :] == wanted
            hits = jnp.where(match, 1.0, hits)
            wt = jnp.where(match, weights[k : k + 1, :], wt)
        rank = jnp.dot(hits.astype(BF16), earlier, preferred_element_type=F32).astype(jnp.int32)
        in_slot = (hits > 0.0) & (rank == slot % cap) & (slot_block == slot // cap % 2)
        row = iota((2 * rows_z, chunk_tok), 0)
        row_block = iota((2 * rows_z, chunk_tok), 1) // tok
        grouped = (routes[0:1, :] // GROUP == z) & (row >= 0)
        g_rank = jnp.dot(
            jnp.where(grouped, 1.0, 0.0).astype(BF16), earlier, preferred_element_type=F32
        ).astype(jnp.int32)
        in_row = grouped & (g_rank == row % rows_z) & (row_block == row // rows_z)
        pick[c] = (
            nt_dot(
                jnp.where(in_slot, 1.0, 0.0).astype(BF16),
                jnp.where(in_row, 1.0, 0.0).astype(BF16),
            )
            .astype(BF16)
            .reshape(n_exp, slots, 2 * rows_z)
        )
        weight = jnp.sum(jnp.where(in_slot, wt, 0.0), axis=1, keepdims=True)
        slot_w[c] = jnp.broadcast_to(weight, (n_slot, 128)).reshape(n_exp, slots, 128)

    make_pick(0)
    pl.semaphore_wait(barrier, 4 + n_z - 1)

    def dispatch(c):
        return remote(
            send_rows.at[c], compact.at[c, core], d_send.at[c], d_recv.at[c, core],
            ep=2 * chip(c) + core,
        )

    def forward(c, block):
        src = send_rows.at[0] if c == 0 else compact.at[c, block]
        return remote(
            src, compact.at[c, block], f_send.at[c], d_recv.at[c, block], ep=partner
        )

    forward(0, core).start()
    for c in range(1, n_z):
        dispatch(c).start()
    compact[0, core] = send_rows[0]

    def square_copy(c, k):
        return remote(
            ss_out.at[c], ss_in.at[c, k], ss_send.at[c, k], ss_recv.at[c, k], tp=peers[k]
        )

    def s1(c, h, k, e):
        return remote(
            part.at[c, h, e], s1_in.at[c, h, k], s1_send.at[c, h, k], s1_recv.at[c, h, k],
            tp=peers[h],
        )

    def s2(c, h):
        return remote(
            s2_out.at[c, h], s2_in.at[c, h], s2_send.at[c, h], s2_recv.at[c, h], tp=peers[1 - h]
        )

    def gather(c, h, k):
        piece = act.at[c, h, tp]
        return remote(piece, piece, g_send.at[c, h, k], g_recv.at[c, h, k], tp=peers[k])

    def relay(c, h):
        piece = act.at[c, h, peers[h]]
        return remote(piece, piece, g_send.at[c, h, 2], g_recv.at[c, h, 2], tp=peers[1 - h])

    def swap(c):
        return remote(x_out.at[c], x_in.at[c], x_send.at[c], x_recv.at[c], ep=partner)

    def home(c):
        return remote(
            r_out.at[c], r_in.at[c], r_send.at[c], r_recv.at[c], ep=2 * chip(c) + core
        )

    def home_square(c, k):
        return remote(
            so_out.at[c], so_in.at[c, k], so_send.at[c, k], so_recv.at[c, k],
            ep=2 * chip(c) + core, tp=(x_tp, y_tp, xy_tp, tp)[k],
        )

    def take_in(c):
        dispatch(c).wait_recv()
        forward(c, core).start()

    def gate_up(c):
        forward(c, other).wait_recv()
        raw = compact[c].reshape(2 * rows_z, width).astype(F32)
        square = jnp.sum(raw * raw, axis=1, keepdims=True)
        diag = iota((2 * rows_z, 128), 0) == iota((2 * rows_z, 128), 1)
        row = jnp.sum(jnp.where(diag, square, 0.0), axis=0, keepdims=True)
        ss_out[c] = jnp.broadcast_to(row, (8, 128))
        for k in range(3):
            square_copy(c, k).start()
        gained = (raw * in_gain_ref[...]).astype(BF16)
        rows[...] = (
            jnp.dot(pick[c].reshape(n_slot, 2 * rows_z), gained, preferred_element_type=F32)
            .astype(BF16)
            .reshape(n_exp, slots, width)
        )

        for p in range(n_exp):
            if p == n_exp - 1 and c + 1 < n_z:
                take_in(c + 1)
            e = expert(p)
            if c == 0:
                w_copy(0, p).wait()
                w_copy(1, p).wait()
            for h in range(2):
                cols = slice(h * half, (h + 1) * half)
                part[c, h, e, :, 0:half] = jnp.dot(
                    rows[e], wg[e, :, cols], preferred_element_type=F32
                ).astype(BF16)
                part[c, h, e, :, half:ff] = jnp.dot(
                    rows[e], wu[e, :, cols], preferred_element_type=F32
                ).astype(BF16)
            if p < 2:
                s1(c, 0, p, e).start()
            if p % 2 == 0:
                s1(c, 1, p // 2, e).start()

    def reduce_first(c):
        for h in range(2):
            e = peers[1 - h]
            s1(c, h, 0, e).wait_recv()
            s2_out[c, h] = (part[c, h, e].astype(F32) + s1_in[c, h, 0].astype(F32)).astype(BF16)
            s2(c, h).start()

    def activate(c):
        for k in range(3):
            square_copy(c, k).wait_recv()
        square = ss_out[c] + ss_in[c, 0] + ss_in[c, 1] + ss_in[c, 2]
        scale_row = lax.rsqrt(square[0:1, 0 : 2 * rows_z] / D + EPS)
        scale = jnp.sum(pick[c, tp].astype(F32) * scale_row, axis=1, keepdims=True)
        weight = slot_w[c, tp][:, 0:1]
        for h in range(2):
            s1(c, h, 1, tp).wait_recv()
            s2(c, h).wait_recv()
            total = (
                part[c, h, tp].astype(F32)
                + s1_in[c, h, 1].astype(F32)
                + s2_in[c, h].astype(F32)
            ) * scale
            gate, up = total[:, 0:half], total[:, half:ff]
            act[c, h, tp] = (gate / (1.0 + jnp.exp(-gate)) * up * weight).astype(BF16)
            gather(c, h, h).start()
        gather(c, 1, 0).start()
        gather(c, 0, 1).start()

    def pass_on(c):
        for h in range(2):
            gather(c, h, h).wait_recv()
            relay(c, h).start()

    def down(c):
        gather(c, 0, 1).wait_recv()
        gather(c, 1, 0).wait_recv()
        for i in range(n_exp):
            p = n_exp - 1 - i
            e = expert(p)
            if i == n_exp - 1:
                for h in range(2):
                    relay(c, h).wait_recv()
            if c == 0:
                w_copy(2, p).wait()
            res[e] = (
                jnp.dot(act[c, 0, e], wd[e, 0:half, :], preferred_element_type=F32)
                + jnp.dot(act[c, 1, e], wd[e, half:ff, :], preferred_element_type=F32)
            ).astype(BF16)

        comb[c] = tdot(
            pick[c].reshape(n_slot, 2 * rows_z), res[...].reshape(n_slot, width)
        ).reshape(2, rows_z, width)
        x_out[c] = comb[c, other].astype(BF16)
        swap(c).start()

    def send_home(c):
        swap(c).wait_recv()
        total = comb[c, core] + x_in[c].astype(F32)
        square = jnp.sum(total * total, axis=1, keepdims=True)
        diag = c * rows_z + iota((rows_z, 128), 0) == iota((rows_z, 128), 1)
        row = jnp.sum(jnp.where(diag, square, 0.0), axis=0, keepdims=True)
        so_out[c] = jnp.broadcast_to(row, (8, 128))
        if c:
            r_out[c] = total.astype(BF16)
            home(c).start()
        else:
            r_in[0] = total.astype(BF16)
            so_in[0, 3] = so_out[0]
        for k in range(4 if c else 3):
            home_square(c, k).start()

    stage = {
        "A": gate_up,
        "B": reduce_first,
        "C": activate,
        "D": pass_on,
        "E": down,
        "F": send_home,
        "P": make_pick,
    }
    for step in ORDER:
        with jax.named_scope(step):
            stage[step[0]](int(step[1]))

    square = so_in[0, 3]
    for c in range(n_z):
        if c:
            home(c).wait_recv()
        for k in range(4 if c else 3):
            home_square(c, k).wait_recv()
            square = square + so_in[c, k]
    combined = jnp.dot(
        own_pick[...], r_in[...].reshape(n_z * rows_z, width), preferred_element_type=F32
    )
    scale_row = lax.rsqrt(square[0:1, :] / D + EPS)
    scale = jnp.sum(own_pick[...].astype(F32) * scale_row, axis=1, keepdims=True)
    out_ref[...] = (combined * scale * out_gain_ref[...]).astype(BF16)

    for c in range(n_z):
        forward(c, core).wait_send()
        if c:
            dispatch(c).wait_send()
            home(c).wait_send()
        for k in range(3):
            square_copy(c, k).wait_send()
        for h in range(2):
            s1(c, h, 0, xy_tp).wait_send()
            s1(c, h, 1, peers[h]).wait_send()
            s2(c, h).wait_send()
            gather(c, h, 0).wait_send()
            gather(c, h, 1).wait_send()
            relay(c, h).wait_send()
        swap(c).wait_send()
        for k in range(4 if c else 3):
            home_square(c, k).wait_send()


def fused(mesh, tokens, in_gain, out_gain, routes, route_weights, w_gate, w_up, w_down):
    tok, width = tokens.shape
    top = routes.shape[1]
    n_exp, _, ff = w_gate.shape
    n_ep = mesh.shape["ep"]
    n_z = n_ep // 2
    cap = max(2, 2 * tok * top // (n_exp * n_ep))
    rows_z = cap * GROUP // top
    slots = 2 * cap
    cfg = (n_z, tok, n_exp, cap, width, ff, top)
    vmem = pl.BlockSpec(memory_space=pltpu.VMEM)
    hbm = pl.BlockSpec(memory_space=pl.ANY)
    dma = pltpu.SemaphoreType.DMA
    return pl.pallas_call(
        functools.partial(kernel, cfg),
        out_shape=jax.ShapeDtypeStruct((tok, width), BF16),
        in_specs=[vmem] * 5 + [hbm] * 3,
        out_specs=vmem,
        scratch_shapes=[
            pltpu.VMEM(w_gate.shape, BF16),
            pltpu.VMEM(w_up.shape, BF16),
            pltpu.VMEM(w_down.shape, BF16),
            pltpu.VMEM((n_z, n_exp, slots, 2 * rows_z), BF16),
            pltpu.VMEM((n_z, n_exp, slots, 128), F32),
            pltpu.VMEM((tok, n_z * rows_z), BF16),
            pltpu.VMEM((n_z, rows_z, width), BF16),
            pltpu.VMEM((n_z, 2, rows_z, width), BF16),
            pltpu.VMEM((n_exp, slots, width), BF16),
            pltpu.VMEM((n_z, 8, 128), F32),
            pltpu.VMEM((n_z, 3, 8, 128), F32),
            pltpu.VMEM((n_z, 2, n_exp, slots, ff), BF16),
            pltpu.VMEM((n_z, 2, 2, slots, ff), BF16),
            pltpu.VMEM((n_z, 2, slots, ff), BF16),
            pltpu.VMEM((n_z, 2, slots, ff), BF16),
            pltpu.VMEM((n_z, 2, n_exp, slots, ff // 2), BF16),
            pltpu.VMEM((n_exp, slots, width), BF16),
            pltpu.VMEM((n_z, 2, rows_z, width), F32),
            pltpu.VMEM((n_z, rows_z, width), BF16),
            pltpu.VMEM((n_z, rows_z, width), BF16),
            pltpu.VMEM((n_z, rows_z, width), BF16),
            pltpu.VMEM((n_z, rows_z, width), BF16),
            pltpu.VMEM((n_z, 8, 128), F32),
            pltpu.VMEM((n_z, 4, 8, 128), F32),
            dma((3, n_exp)),
            dma((n_z,)),
            dma((n_z, 2)),
            dma((n_z,)),
            dma((n_z, 3)),
            dma((n_z, 3)),
            dma((n_z, 2, 2)),
            dma((n_z, 2, 2)),
            dma((n_z, 2)),
            dma((n_z, 2)),
            dma((n_z, 2, 3)),
            dma((n_z, 2, 3)),
            dma((n_z,)),
            dma((n_z,)),
            dma((n_z,)),
            dma((n_z,)),
            dma((n_z, 4)),
            dma((n_z, 4)),
        ],
        compiler_params=pltpu.CompilerParams(
            collective_id=0, has_side_effects=True, vmem_limit_bytes=60 * 2**20
        ),
    )(
        tokens,
        in_gain.reshape(1, width),
        out_gain.reshape(1, width),
        routes.T,
        route_weights.T,
        w_gate,
        w_up,
        w_down,
    )


def run_experts(slot_rows, w_gate, w_up, w_down):
    gate_part = jnp.einsum(
        "secd,edf->secf", slot_rows, w_gate, preferred_element_type=jnp.float32
    ).astype(jnp.bfloat16)
    up_part = jnp.einsum(
        "secd,edf->secf", slot_rows, w_up, preferred_element_type=jnp.float32
    ).astype(jnp.bfloat16)
    gate_sum, up_sum = (
        lax.psum(gate_part, "tp").astype(jnp.float32),
        lax.psum(up_part, "tp").astype(jnp.float32),
    )
    active = (jax.nn.silu(gate_sum) * up_sum).astype(jnp.bfloat16)
    return jnp.einsum("secf,efd->secd", active, w_down, preferred_element_type=jnp.float32).astype(
        jnp.bfloat16
    )


def on_device(tokens, in_gain, out_gain, routes, route_weights, w_gate, w_up, w_down):
    tok_rows, local_width = tokens.shape
    top_count = routes.shape[1]
    local_experts = w_gate.shape[0]
    groups_ep = lax.axis_size("ep")
    experts = local_experts * groups_ep
    capacity = max(2, 2 * tok_rows * top_count // experts)
    values = tokens.astype(jnp.float32)
    sum_squares = lax.psum(jnp.sum(values * values, axis=1), "tp")
    normed = (values * lax.rsqrt(sum_squares / D + EPS)[:, None] * in_gain).astype(jnp.bfloat16)
    row_start = lax.axis_index("ep") * tok_rows
    my_routes = lax.dynamic_slice_in_dim(routes, row_start, tok_rows, 0)
    my_weights = lax.dynamic_slice_in_dim(route_weights, row_start, tok_rows, 0)
    flat_ids = my_routes.reshape(-1)
    matches = (flat_ids[:, None] == jnp.arange(experts, dtype=jnp.int32)[None, :]).astype(jnp.int32)
    slot_rank = jnp.sum((jnp.cumsum(matches, axis=0) - matches) * matches, axis=1)
    position = flat_ids * capacity + slot_rank
    dispatch_table = jnp.any(
        position.reshape(tok_rows, top_count, 1)
        == jnp.arange(experts * capacity, dtype=jnp.int32)[None, None, :],
        axis=1,
    )
    outgoing = jnp.einsum(
        "ts,td->sd", dispatch_table.astype(jnp.bfloat16), normed, preferred_element_type=jnp.float32
    ).astype(jnp.bfloat16)
    outgoing = outgoing.reshape(groups_ep, local_experts, capacity, local_width)
    answers = run_experts(
        lax.all_to_all(outgoing, "ep", split_axis=0, concat_axis=0, tiled=True),
        w_gate,
        w_up,
        w_down,
    )
    returned = lax.all_to_all(answers, "ep", split_axis=0, concat_axis=0, tiled=True)
    flat_out = returned.reshape(experts * capacity, local_width)
    picked = flat_out[position].reshape(tok_rows, top_count, local_width)
    combined = jnp.sum(my_weights[:, :, None] * picked.astype(jnp.float32), axis=1)
    out_squares = lax.psum(jnp.sum(combined * combined, axis=1), "tp")
    return (combined * lax.rsqrt(out_squares / D + EPS)[:, None] * out_gain).astype(jnp.bfloat16)


def solution(mesh):
    placed = (
        P("ep", "tp"),
        P("tp"),
        P("tp"),
        P(),
        P(),
        P("ep", "tp", None),
        P("ep", "tp", None),
        P("ep", None, "tp"),
    )
    body = on_device
    if mesh.shape["tp"] == 4 and mesh.shape["ep"] == 8:
        body = functools.partial(fused, mesh)
    return jax.shard_map(
        body, mesh=mesh, in_specs=placed, out_specs=P("ep", "tp"), check_vma=False
    )
```

```python
import functools

import jax
import jax.numpy as jnp
from jax import lax
from jax.experimental import pallas as pl
from jax.experimental.pallas import tpu as pltpu
from jax.sharding import PartitionSpec as P

D = 4096
GROUP = 8

EPS = 1e-06
MESH = pl.DeviceIdType.MESH
F32, BF16 = jnp.float32, jnp.bfloat16

ORDER = (
    "P1", "P2", "P3", "A00", "A01", "A02", "N1", "A03", "A10", "A11", "N2", "B00", "A12", "A13",
    "N3", "B01", "A20", "A21", "A22", "A23", "A30", "B20", "B21", "A31", "A32", "A33", "B30", "B31",
    "C20", "C21", "B11", "B10", "C30", "C31", "D21", "C00", "D20", "E20", "E21", "C01", "C10", "C11",
    "D30", "E30", "E31", "E32", "D31", "E22", "E23", "D01", "D00", "E00", "E01", "D11", "D10", "F2",
    "E10", "E11", "E33", "E12", "F3", "E13", "E02", "E03", "F1", "F0",
)


def iota(shape, dim):
    return lax.broadcasted_iota(jnp.int32, shape, dim)


def tdot(a, b):
    return lax.dot_general(a, b, (((0,), (0,)), ((), ())), preferred_element_type=F32)


def kernel(
    cfg,
    tokens_ref,
    in_gain_ref,
    out_gain_ref,
    routes_ref,
    weights_ref,
    wg_hbm,
    wu_hbm,
    wd_hbm,
    out_ref,
    wg,
    wu,
    wd,
    pick,
    slot_w,
    own_pick,
    send_rows,
    compact,
    rows,
    ss_out,
    ss_in,
    part,
    s1_in,
    s2_out,
    s2_in,
    act,
    res,
    wide,
    comb,
    x_out,
    x_in,
    r_out,
    r_in,
    so_out,
    so_in,
    w_sem,
    d_send,
    d_recv,
    f_send,
    ss_send,
    ss_recv,
    s1_send,
    s1_recv,
    s2_send,
    s2_recv,
    g_send,
    g_recv,
    x_send,
    x_recv,
    r_send,
    r_recv,
    so_send,
    so_recv,
):
    n_z, tok, n_exp, cap, width, ff, top = cfg
    rows_z = cap * GROUP // top
    half = ff // 2
    slots = 2 * cap
    me = lax.axis_index("ep")
    tp = lax.axis_index("tp")
    z, core = me // 2, lax.rem(me, 2)
    other = 1 - core
    y, x = tp // 2, lax.rem(tp, 2)
    x_tp = 2 * y + (1 - x)
    y_tp = 2 * (1 - y) + x
    xy_tp = 2 * (1 - y) + (1 - x)
    partner = 2 * z + other
    peers = (x_tp, y_tp, xy_tp)

    def expert(p):
        return 2 * lax.rem(y + 1 - p % 2, 2) + lax.rem(x + 1 - p // 2, 2)

    def chip(c):
        return 2 * ((z // 2 + c // 2) % 2) + (z % 2 + c % 2 + c // 2) % 2

    def w_copy(k, p):
        hbm, vmem = ((wg_hbm, wg), (wu_hbm, wu), (wd_hbm, wd))[k]
        e = expert(p)
        return pltpu.make_async_copy(hbm.at[e], vmem.at[e], w_sem.at[k, p])

    for p in range(n_exp):
        w_copy(0, p).start()
        w_copy(1, p).start()
    for p in reversed(range(n_exp)):
        w_copy(2, p).start()

    barrier = pltpu.get_barrier_semaphore()
    for c in range(1, n_z):
        pl.semaphore_signal(
            barrier, inc=1, device_id={"ep": 2 * chip(c) + core}, device_id_type=MESH
        )
    for peer in peers:
        pl.semaphore_signal(barrier, inc=1, device_id={"tp": peer}, device_id_type=MESH)
    pl.semaphore_signal(barrier, inc=1, device_id={"ep": partner}, device_id_type=MESH)

    def remote(src, dst, send, recv, **dev):
        return pltpu.make_async_remote_copy(
            src_ref=src,
            dst_ref=dst,
            send_sem=send,
            recv_sem=recv,
            device_id=dev,
            device_id_type=MESH,
        )

    chunk_tok = 2 * tok
    n_slot = n_exp * slots
    n_row = n_z * rows_z

    def nt_dot(a, b):
        return lax.dot_general(a, b, (((1,), (1,)), ((), ())), preferred_element_type=F32)

    def chip_tokens(ref, c):
        return ref[:, pl.ds(pl.multiple_of(chip(c) * chunk_tok, chunk_tok), chunk_tok)]

    both = chip_tokens(routes_ref, 0)[0:1, :]
    group = jnp.where(core == 0, both[:, 0:tok], both[:, tok:chunk_tok]) // GROUP
    row_of = iota((n_row, tok), 0)
    hit = group == chip(row_of // rows_z)
    earlier = jnp.where(iota((tok, tok), 0) < iota((tok, tok), 1), 1.0, 0.0).astype(BF16)
    rank = jnp.dot(
        jnp.where(hit, 1.0, 0.0).astype(BF16), earlier, preferred_element_type=F32
    ).astype(jnp.int32)
    own = jnp.where(hit & (rank == row_of % rows_z), 1.0, 0.0)
    send_rows[...] = (
        jnp.dot(own.astype(BF16), tokens_ref[...], preferred_element_type=F32)
        .astype(BF16)
        .reshape(n_z, rows_z, width)
    )
    own_pick[...] = own.T.astype(BF16)

    def make_pick(c):
        routes = chip_tokens(routes_ref, c)
        weights = chip_tokens(weights_ref, c)
        t_row, t_col = iota((chunk_tok, chunk_tok), 0), iota((chunk_tok, chunk_tok), 1)
        earlier = jnp.where((t_row < t_col) & (t_col // tok == t_row // tok), 1.0, 0.0).astype(BF16)
        slot = iota((n_slot, chunk_tok), 0)
        slot_block = iota((n_slot, chunk_tok), 1) // tok
        wanted = me * n_exp + slot // slots
        hits = jnp.zeros((n_slot, chunk_tok), F32)
        wt = jnp.zeros((n_slot, chunk_tok), F32)
        for k in range(top):
            match = routes[k : k + 1, :] == wanted
            hits = jnp.where(match, 1.0, hits)
            wt = jnp.where(match, weights[k : k + 1, :], wt)
        rank = jnp.dot(hits.astype(BF16), earlier, preferred_element_type=F32).astype(jnp.int32)
        in_slot = (hits > 0.0) & (rank == slot % cap) & (slot_block == slot // cap % 2)
        row = iota((2 * rows_z, chunk_tok), 0)
        row_block = iota((2 * rows_z, chunk_tok), 1) // tok
        grouped = (routes[0:1, :] // GROUP == z) & (row >= 0)
        g_rank = jnp.dot(
            jnp.where(grouped, 1.0, 0.0).astype(BF16), earlier, preferred_element_type=F32
        ).astype(jnp.int32)
        in_row = grouped & (g_rank == row % rows_z) & (row_block == row // rows_z)
        pick[c] = (
            nt_dot(
                jnp.where(in_slot, 1.0, 0.0).astype(BF16),
                jnp.where(in_row, 1.0, 0.0).astype(BF16),
            )
            .astype(BF16)
            .reshape(n_exp, slots, 2 * rows_z)
        )
        weight = jnp.sum(jnp.where(in_slot, wt, 0.0), axis=1, keepdims=True)
        slot_w[c] = jnp.broadcast_to(weight, (n_slot, 128)).reshape(n_exp, slots, 128)

    make_pick(0)
    pl.semaphore_wait(barrier, 4 + n_z - 1)

    def dispatch(c):
        return remote(
            send_rows.at[c], compact.at[c, core], d_send.at[c], d_recv.at[c, core],
            ep=2 * chip(c) + core,
        )

    def forward(c, block):
        src = send_rows.at[0] if c == 0 else compact.at[c, block]
        return remote(
            src, compact.at[c, block], f_send.at[c], d_recv.at[c, block], ep=partner
        )

    forward(0, core).start()
    for c in range(1, n_z):
        dispatch(c).start()
    compact[0, core] = send_rows[0]

    def square_copy(c, k):
        return remote(
            ss_out.at[c], ss_in.at[c, k], ss_send.at[c, k], ss_recv.at[c, k], tp=peers[k]
        )

    def mine(c, h, p):
        first = pl.multiple_of(expert(p) * slots, slots)
        return part.at[c, h, p, pl.ds(first, slots)]

    def s1(c, h, k, p):
        return remote(
            mine(c, h, p), s1_in.at[c, h, k], s1_send.at[c, h, k], s1_recv.at[c, h, k],
            tp=peers[h],
        )

    def s2(c, h):
        return remote(
            s2_out.at[c, h], s2_in.at[c, h], s2_send.at[c, h], s2_recv.at[c, h], tp=peers[1 - h]
        )

    def gather(c, h, k):
        piece = act.at[c, h, tp]
        return remote(piece, piece, g_send.at[c, h, k], g_recv.at[c, h, k], tp=peers[k])

    def relay(c, h):
        piece = act.at[c, h, peers[h]]
        return remote(piece, piece, g_send.at[c, h, 2], g_recv.at[c, h, 2], tp=peers[1 - h])

    def swap(c):
        return remote(x_out.at[c], x_in.at[c], x_send.at[c], x_recv.at[c], ep=partner)

    def home(c):
        return remote(
            r_out.at[c], r_in.at[c], r_send.at[c], r_recv.at[c], ep=2 * chip(c) + core
        )

    def home_square(c, k):
        return remote(
            so_out.at[c], so_in.at[c, k], so_send.at[c, k], so_recv.at[c, k],
            ep=2 * chip(c) + core, tp=(x_tp, y_tp, xy_tp, tp)[k],
        )

    def take_in(c):
        dispatch(c).wait_recv()
        forward(c, core).start()

    waited = set()

    def arrive(copy, *which):
        if (copy, which) not in waited:
            waited.add((copy, which))
            copy(*which).wait_recv()

    def gate_up(c, p):
        if p == 0:
            forward(c, other).wait_recv()
            raw = compact[c].reshape(2 * rows_z, width).astype(F32)
            square = jnp.sum(raw * raw, axis=1, keepdims=True)
            diag = iota((2 * rows_z, 128), 0) == iota((2 * rows_z, 128), 1)
            row = jnp.sum(jnp.where(diag, square, 0.0), axis=0, keepdims=True)
            ss_out[c] = jnp.broadcast_to(row, (8, 128))
            for k in range(3):
                square_copy(c, k).start()
            gained = (raw * in_gain_ref[...]).astype(BF16)
            rows[c] = (
                jnp.dot(pick[c].reshape(n_slot, 2 * rows_z), gained, preferred_element_type=F32)
                .astype(BF16)
            )
        e = expert(p)
        if c == 0:
            w_copy(0, p).wait()
            w_copy(1, p).wait()
        for h in range(2):
            cols = slice(h * half, (h + 1) * half)
            part[c, h, p, :, 0:half] = jnp.dot(
                rows[c], wg[e, :, cols], preferred_element_type=F32
            ).astype(BF16)
            part[c, h, p, :, half:ff] = jnp.dot(
                rows[c], wu[e, :, cols], preferred_element_type=F32
            ).astype(BF16)
        if p < 2:
            s1(c, 0, p, p).start()
        if p % 2 == 0:
            s1(c, 1, p // 2, p).start()

    def reduce_first(c, h):
        s1(c, h, 0, 0).wait_recv()
        s2_out[c, h] = (mine(c, h, 2 - h)[...].astype(F32) + s1_in[c, h, 0].astype(F32)).astype(BF16)
        s2(c, h).start()

    def activate(c, h):
        for k in range(3):
            arrive(square_copy, c, k)
        square = ss_out[c] + ss_in[c, 0] + ss_in[c, 1] + ss_in[c, 2]
        scale_row = lax.rsqrt(square[0:1, 0 : 2 * rows_z] / D + EPS)
        scale = jnp.sum(pick[c, tp].astype(F32) * scale_row, axis=1, keepdims=True)
        weight = slot_w[c, tp][:, 0:1]
        s1(c, h, 1, 3).wait_recv()
        s2(c, h).wait_recv()
        total = (
            mine(c, h, 3)[...].astype(F32) + s1_in[c, h, 1].astype(F32) + s2_in[c, h].astype(F32)
        ) * scale
        gate, up = total[:, 0:half], total[:, half:ff]
        act[c, h, tp] = (gate / (1.0 + jnp.exp(-gate)) * up * weight).astype(BF16)
        gather(c, h, h).start()
        if h == 1:
            gather(c, 1, 0).start()
            gather(c, 0, 1).start()

    def pass_on(c, h):
        arrive(gather, c, h, h)
        relay(c, h).start()

    def down(c, i):
        p = (3, 1, 2, 0)[i]
        e = expert(p)
        for h in range(2):
            if i == n_exp - 1:
                relay(c, h).wait_recv()
            elif i:
                arrive(gather, c, h, i - 1)
        if ("down", p) not in waited:
            waited.add(("down", p))
            w_copy(2, p).wait()
        wide[...] = (
            jnp.dot(jnp.concatenate([act[c, 0, e]] * 4), wd[e, 0:half], preferred_element_type=F32)
            + jnp.dot(jnp.concatenate([act[c, 1, e]] * 4), wd[e, half:], preferred_element_type=F32)
        ).astype(BF16)
        res[c, e] = wide[0:slots]
        if i == n_exp - 1:
            comb[c] = tdot(
                pick[c].reshape(n_slot, 2 * rows_z), res[c].reshape(n_slot, width)
            ).reshape(2, rows_z, width)
            x_out[c] = comb[c, other].astype(BF16)
            swap(c).start()

    def send_home(c):
        swap(c).wait_recv()
        total = comb[c, core] + x_in[c].astype(F32)
        square = jnp.sum(total * total, axis=1, keepdims=True)
        diag = c * rows_z + iota((rows_z, 128), 0) == iota((rows_z, 128), 1)
        row = jnp.sum(jnp.where(diag, square, 0.0), axis=0, keepdims=True)
        so_out[c] = jnp.broadcast_to(row, (8, 128))
        for k in range(4 if c else 3):
            home_square(c, k).start()
        if c:
            r_out[c] = total.astype(BF16)
            home(c).start()
        else:
            r_in[0] = total.astype(BF16)
            so_in[0, 3] = so_out[0]

    stage = {
        "A": gate_up,
        "B": reduce_first,
        "C": activate,
        "D": pass_on,
        "E": down,
        "F": send_home,
        "N": take_in,
        "P": make_pick,
    }
    for step in ORDER:
        with jax.named_scope(step):
            stage[step[0]](*(int(digit) for digit in step[1:]))

    for c in range(n_z):
        forward(c, core).wait_send()
        if c:
            dispatch(c).wait_send()
        for k in range(3):
            square_copy(c, k).wait_send()
        for h in range(2):
            s1(c, h, 0, 0).wait_send()
            s1(c, h, 1, 1 + h).wait_send()
            s2(c, h).wait_send()
            gather(c, h, 0).wait_send()
            gather(c, h, 1).wait_send()
            relay(c, h).wait_send()
        swap(c).wait_send()

    square = so_in[0, 3]
    for c in range(n_z):
        if c:
            home(c).wait_recv()
        for k in range(4 if c else 3):
            home_square(c, k).wait_recv()
            square = square + so_in[c, k]
    combined = jnp.dot(
        own_pick[...], r_in[...].reshape(n_z * rows_z, width), preferred_element_type=F32
    )
    scale_row = lax.rsqrt(square[0:1, :] / D + EPS)
    scale = jnp.sum(own_pick[...].astype(F32) * scale_row, axis=1, keepdims=True)
    out_ref[...] = (combined * scale * out_gain_ref[...]).astype(BF16)

    for c in range(n_z):
        if c:
            home(c).wait_send()
        for k in range(4 if c else 3):
            home_square(c, k).wait_send()


def fused(mesh, tokens, in_gain, out_gain, routes, route_weights, w_gate, w_up, w_down):
    tok, width = tokens.shape
    top = routes.shape[1]
    n_exp, _, ff = w_gate.shape
    n_ep = mesh.shape["ep"]
    n_z = n_ep // 2
    cap = max(2, 2 * tok * top // (n_exp * n_ep))
    rows_z = cap * GROUP // top
    slots = 2 * cap
    cfg = (n_z, tok, n_exp, cap, width, ff, top)
    vmem = pl.BlockSpec(memory_space=pltpu.VMEM)
    hbm = pl.BlockSpec(memory_space=pl.ANY)
    dma = pltpu.SemaphoreType.DMA
    return pl.pallas_call(
        functools.partial(kernel, cfg),
        out_shape=jax.ShapeDtypeStruct((tok, width), BF16),
        in_specs=[vmem] * 5 + [hbm] * 3,
        out_specs=vmem,
        scratch_shapes=[
            pltpu.VMEM(w_gate.shape, BF16),
            pltpu.VMEM(w_up.shape, BF16),
            pltpu.VMEM(w_down.shape, BF16),
            pltpu.VMEM((n_z, n_exp, slots, 2 * rows_z), BF16),
            pltpu.VMEM((n_z, n_exp, slots, 128), F32),
            pltpu.VMEM((tok, n_z * rows_z), BF16),
            pltpu.VMEM((n_z, rows_z, width), BF16),
            pltpu.VMEM((n_z, 2, rows_z, width), BF16),
            pltpu.VMEM((n_z, n_exp * slots, width), BF16),
            pltpu.VMEM((n_z, 8, 128), F32),
            pltpu.VMEM((n_z, 3, 8, 128), F32),
            pltpu.VMEM((n_z, 2, n_exp, n_exp * slots, ff), BF16),
            pltpu.VMEM((n_z, 2, 2, slots, ff), BF16),
            pltpu.VMEM((n_z, 2, slots, ff), BF16),
            pltpu.VMEM((n_z, 2, slots, ff), BF16),
            pltpu.VMEM((n_z, 2, n_exp, slots, ff // 2), BF16),
            pltpu.VMEM((n_z, n_exp, slots, width), BF16),
            pltpu.VMEM((4 * slots, width), BF16),
            pltpu.VMEM((n_z, 2, rows_z, width), F32),
            pltpu.VMEM((n_z, rows_z, width), BF16),
            pltpu.VMEM((n_z, rows_z, width), BF16),
            pltpu.VMEM((n_z, rows_z, width), BF16),
            pltpu.VMEM((n_z, rows_z, width), BF16),
            pltpu.VMEM((n_z, 8, 128), F32),
            pltpu.VMEM((n_z, 4, 8, 128), F32),
            dma((3, n_exp)),
            dma((n_z,)),
            dma((n_z, 2)),
            dma((n_z,)),
            dma((n_z, 3)),
            dma((n_z, 3)),
            dma((n_z, 2, 2)),
            dma((n_z, 2, 2)),
            dma((n_z, 2)),
            dma((n_z, 2)),
            dma((n_z, 2, 3)),
            dma((n_z, 2, 3)),
            dma((n_z,)),
            dma((n_z,)),
            dma((n_z,)),
            dma((n_z,)),
            dma((n_z, 4)),
            dma((n_z, 4)),
        ],
        compiler_params=pltpu.CompilerParams(
            collective_id=0, has_side_effects=True, vmem_limit_bytes=52 * 2**20
        ),
    )(
        *(
            pltpu.with_memory_space_constraint(array, pltpu.HBM)
            for array in (
                tokens,
                in_gain.reshape(1, width),
                out_gain.reshape(1, width),
                routes.T,
                route_weights.T,
                w_gate,
                w_up,
                w_down,
            )
        )
    )


def run_experts(slot_rows, w_gate, w_up, w_down):
    gate_part = jnp.einsum(
        "secd,edf->secf", slot_rows, w_gate, preferred_element_type=jnp.float32
    ).astype(jnp.bfloat16)
    up_part = jnp.einsum(
        "secd,edf->secf", slot_rows, w_up, preferred_element_type=jnp.float32
    ).astype(jnp.bfloat16)
    gate_sum, up_sum = (
        lax.psum(gate_part, "tp").astype(jnp.float32),
        lax.psum(up_part, "tp").astype(jnp.float32),
    )
    active = (jax.nn.silu(gate_sum) * up_sum).astype(jnp.bfloat16)
    return jnp.einsum("secf,efd->secd", active, w_down, preferred_element_type=jnp.float32).astype(
        jnp.bfloat16
    )


def on_device(tokens, in_gain, out_gain, routes, route_weights, w_gate, w_up, w_down):
    tok_rows, local_width = tokens.shape
    top_count = routes.shape[1]
    local_experts = w_gate.shape[0]
    groups_ep = lax.axis_size("ep")
    experts = local_experts * groups_ep
    capacity = max(2, 2 * tok_rows * top_count // experts)
    values = tokens.astype(jnp.float32)
    sum_squares = lax.psum(jnp.sum(values * values, axis=1), "tp")
    normed = (values * lax.rsqrt(sum_squares / D + EPS)[:, None] * in_gain).astype(jnp.bfloat16)
    row_start = lax.axis_index("ep") * tok_rows
    my_routes = lax.dynamic_slice_in_dim(routes, row_start, tok_rows, 0)
    my_weights = lax.dynamic_slice_in_dim(route_weights, row_start, tok_rows, 0)
    flat_ids = my_routes.reshape(-1)
    matches = (flat_ids[:, None] == jnp.arange(experts, dtype=jnp.int32)[None, :]).astype(jnp.int32)
    slot_rank = jnp.sum((jnp.cumsum(matches, axis=0) - matches) * matches, axis=1)
    position = flat_ids * capacity + slot_rank
    dispatch_table = jnp.any(
        position.reshape(tok_rows, top_count, 1)
        == jnp.arange(experts * capacity, dtype=jnp.int32)[None, None, :],
        axis=1,
    )
    outgoing = jnp.einsum(
        "ts,td->sd", dispatch_table.astype(jnp.bfloat16), normed, preferred_element_type=jnp.float32
    ).astype(jnp.bfloat16)
    outgoing = outgoing.reshape(groups_ep, local_experts, capacity, local_width)
    answers = run_experts(
        lax.all_to_all(outgoing, "ep", split_axis=0, concat_axis=0, tiled=True),
        w_gate,
        w_up,
        w_down,
    )
    returned = lax.all_to_all(answers, "ep", split_axis=0, concat_axis=0, tiled=True)
    flat_out = returned.reshape(experts * capacity, local_width)
    picked = flat_out[position].reshape(tok_rows, top_count, local_width)
    combined = jnp.sum(my_weights[:, :, None] * picked.astype(jnp.float32), axis=1)
    out_squares = lax.psum(jnp.sum(combined * combined, axis=1), "tp")
    return (combined * lax.rsqrt(out_squares / D + EPS)[:, None] * out_gain).astype(jnp.bfloat16)


def solution(mesh):
    placed = (
        P("ep", "tp"),
        P("tp"),
        P("tp"),
        P(),
        P(),
        P("ep", "tp", None),
        P("ep", "tp", None),
        P("ep", None, "tp"),
    )
    body = on_device
    if mesh.shape["tp"] == 4 and mesh.shape["ep"] == 8:
        body = functools.partial(fused, mesh)
    return jax.shard_map(
        body, mesh=mesh, in_specs=placed, out_specs=P("ep", "tp"), check_vma=False
    )
```

```python
import functools

import jax
import jax.numpy as jnp
from jax import lax
from jax.experimental import pallas as pl
from jax.experimental.pallas import tpu as pltpu
from jax.sharding import PartitionSpec as P

D = 4096
GROUP = 8

EPS = 1e-06
MESH = pl.DeviceIdType.MESH
F32, BF16 = jnp.float32, jnp.bfloat16

ORDER = (
    "P0", "P1", "P2", "P3", "A00", "A01", "A02", "N1", "A03", "A10", "A11", "N2", "B00", "A12",
    "A13", "N3", "B01", "A20", "A21", "A22", "A23", "A30", "B20", "B21", "A31", "A32", "A33", "B30",
    "B31", "C20", "C21", "B11", "B10", "C30", "C31", "D21", "C00", "D20", "E20", "E21", "C01", "C10",
    "C11", "D30", "E30", "E31", "E32", "D31", "E22", "E23", "D01", "D00", "E00", "E01", "D11", "D10",
    "F2", "E10", "E11", "E33", "E12", "F3", "E13", "E02", "E03", "F1", "F0",
)


def iota(shape, dim):
    return lax.broadcasted_iota(jnp.int32, shape, dim)


def tdot(a, b):
    return lax.dot_general(a, b, (((0,), (0,)), ((), ())), preferred_element_type=F32)


def kernel(
    cfg,
    tokens_hbm,
    in_gain_hbm,
    out_gain_hbm,
    routes_hbm,
    weights_hbm,
    wg_hbm,
    wu_hbm,
    wd_hbm,
    out_ref,
    tokens_ref,
    in_gain_ref,
    out_gain_ref,
    routes_ref,
    weights_ref,
    wg,
    wu,
    wd,
    pick,
    slot_w,
    own_pick,
    send_rows,
    compact,
    rows,
    ss_out,
    ss_in,
    part,
    s1_in,
    s2_out,
    s2_in,
    act,
    res,
    wide,
    comb,
    combined,
    x_out,
    x_in,
    r_out,
    r_in,
    so_out,
    so_in,
    in_sem,
    w_sem,
    d_send,
    d_recv,
    f_send,
    ss_send,
    ss_recv,
    s1_send,
    s1_recv,
    s2_send,
    s2_recv,
    g_send,
    g_recv,
    x_send,
    x_recv,
    r_send,
    r_recv,
    so_send,
    so_recv,
):
    n_z, tok, n_exp, cap, width, ff, top = cfg
    rows_z = cap * GROUP // top
    half = ff // 2
    slots = 2 * cap
    me = lax.axis_index("ep")
    tp = lax.axis_index("tp")
    z, core = me // 2, lax.rem(me, 2)
    other = 1 - core
    y, x = tp // 2, lax.rem(tp, 2)
    x_tp = 2 * y + (1 - x)
    y_tp = 2 * (1 - y) + x
    xy_tp = 2 * (1 - y) + (1 - x)
    partner = 2 * z + other
    peers = (x_tp, y_tp, xy_tp)

    def expert(p):
        return 2 * lax.rem(y + 1 - p % 2, 2) + lax.rem(x + 1 - p // 2, 2)

    def chip(c):
        return 2 * ((z // 2 + c // 2) % 2) + (z % 2 + c % 2 + c // 2) % 2

    def w_copy(k, p):
        hbm, vmem = ((wg_hbm, wg), (wu_hbm, wu), (wd_hbm, wd))[k]
        e = expert(p)
        return pltpu.make_async_copy(hbm.at[e], vmem.at[e], w_sem.at[k, p])

    barrier = pltpu.get_barrier_semaphore()
    for c in range(1, n_z):
        pl.semaphore_signal(
            barrier, inc=1, device_id={"ep": 2 * chip(c) + core}, device_id_type=MESH
        )
    for peer in peers:
        pl.semaphore_signal(barrier, inc=1, device_id={"tp": peer}, device_id_type=MESH)
    pl.semaphore_signal(barrier, inc=1, device_id={"ep": partner}, device_id_type=MESH)

    copies_in = [
        pltpu.make_async_copy(hbm, vmem, in_sem.at[k])
        for k, (hbm, vmem) in enumerate(
            (
                (routes_hbm, routes_ref),
                (tokens_hbm, tokens_ref),
                (weights_hbm, weights_ref),
                (in_gain_hbm, in_gain_ref),
                (out_gain_hbm, out_gain_ref),
            )
        )
    ]
    for copy in copies_in:
        copy.start()

    def remote(src, dst, send, recv, **dev):
        return pltpu.make_async_remote_copy(
            src_ref=src,
            dst_ref=dst,
            send_sem=send,
            recv_sem=recv,
            device_id=dev,
            device_id_type=MESH,
        )

    chunk_tok = 2 * tok
    n_slot = n_exp * slots
    n_row = n_z * rows_z

    def nt_dot(a, b):
        return lax.dot_general(a, b, (((1,), (1,)), ((), ())), preferred_element_type=F32)

    def chip_tokens(ref, c):
        return ref[:, pl.ds(pl.multiple_of(chip(c) * chunk_tok, chunk_tok), chunk_tok)]

    for copy in copies_in:
        copy.wait()
    for p in range(n_exp):
        w_copy(0, p).start()
        w_copy(1, p).start()
    for p in reversed(range(n_exp)):
        w_copy(2, p).start()

    both = chip_tokens(routes_ref, 0)[0:1, :]
    group = jnp.where(core == 0, both[:, 0:tok], both[:, tok:chunk_tok]) // GROUP
    row_of = iota((n_row, tok), 0)
    hit = group == chip(row_of // rows_z)
    earlier = jnp.where(iota((tok, tok), 0) < iota((tok, tok), 1), 1.0, 0.0).astype(BF16)
    rank = jnp.dot(
        jnp.where(hit, 1.0, 0.0).astype(BF16), earlier, preferred_element_type=F32
    ).astype(jnp.int32)
    own = jnp.where(hit & (rank == row_of % rows_z), 1.0, 0.0)
    send_rows[...] = (
        jnp.dot(own.astype(BF16), tokens_ref[...], preferred_element_type=F32)
        .astype(BF16)
        .reshape(n_z, rows_z, width)
    )

    def make_pick(c):
        routes = chip_tokens(routes_ref, c)
        weights = chip_tokens(weights_ref, c)
        t_row, t_col = iota((chunk_tok, chunk_tok), 0), iota((chunk_tok, chunk_tok), 1)
        earlier = jnp.where((t_row < t_col) & (t_col // tok == t_row // tok), 1.0, 0.0).astype(BF16)
        slot = iota((n_slot, chunk_tok), 0)
        slot_block = iota((n_slot, chunk_tok), 1) // tok
        wanted = me * n_exp + slot // slots
        hits = jnp.zeros((n_slot, chunk_tok), F32)
        wt = jnp.zeros((n_slot, chunk_tok), F32)
        for k in range(top):
            match = routes[k : k + 1, :] == wanted
            hits = jnp.where(match, 1.0, hits)
            wt = jnp.where(match, weights[k : k + 1, :], wt)
        rank = jnp.dot(hits.astype(BF16), earlier, preferred_element_type=F32).astype(jnp.int32)
        in_slot = (hits > 0.0) & (rank == slot % cap) & (slot_block == slot // cap % 2)
        row = iota((2 * rows_z, chunk_tok), 0)
        row_block = iota((2 * rows_z, chunk_tok), 1) // tok
        grouped = (routes[0:1, :] // GROUP == z) & (row >= 0)
        g_rank = jnp.dot(
            jnp.where(grouped, 1.0, 0.0).astype(BF16), earlier, preferred_element_type=F32
        ).astype(jnp.int32)
        in_row = grouped & (g_rank == row % rows_z) & (row_block == row // rows_z)
        pick[c] = (
            nt_dot(
                jnp.where(in_slot, 1.0, 0.0).astype(BF16),
                jnp.where(in_row, 1.0, 0.0).astype(BF16),
            )
            .astype(BF16)
            .reshape(n_exp, slots, 2 * rows_z)
        )
        weight = jnp.sum(jnp.where(in_slot, wt, 0.0), axis=1, keepdims=True)
        slot_w[c] = jnp.broadcast_to(weight, (n_slot, 128)).reshape(n_exp, slots, 128)

    pl.semaphore_wait(barrier, 4 + n_z - 1)

    def dispatch(c):
        return remote(
            send_rows.at[c], compact.at[c, core], d_send.at[c], d_recv.at[c, core],
            ep=2 * chip(c) + core,
        )

    def forward(c, block):
        src = send_rows.at[0] if c == 0 else compact.at[c, block]
        return remote(
            src, compact.at[c, block], f_send.at[c], d_recv.at[c, block], ep=partner
        )

    forward(0, core).start()
    for c in range(1, n_z):
        dispatch(c).start()
    compact[0, core] = send_rows[0]
    own_pick[...] = own.T.astype(BF16)

    def square_copy(c, k):
        return remote(
            ss_out.at[c], ss_in.at[c, k], ss_send.at[c, k], ss_recv.at[c, k], tp=peers[k]
        )

    def mine(c, h, p):
        first = pl.multiple_of(expert(p) * slots, slots)
        return part.at[c, h, p, pl.ds(first, slots)]

    def s1(c, h, k, p):
        return remote(
            mine(c, h, p), s1_in.at[c, h, k], s1_send.at[c, h, k], s1_recv.at[c, h, k],
            tp=peers[h],
        )

    def s2(c, h):
        return remote(
            s2_out.at[c, h], s2_in.at[c, h], s2_send.at[c, h], s2_recv.at[c, h], tp=peers[1 - h]
        )

    def gather(c, h, k):
        piece = act.at[c, h, tp]
        return remote(piece, piece, g_send.at[c, h, k], g_recv.at[c, h, k], tp=peers[k])

    def relay(c, h):
        piece = act.at[c, h, peers[h]]
        return remote(piece, piece, g_send.at[c, h, 2], g_recv.at[c, h, 2], tp=peers[1 - h])

    def swap(c):
        return remote(x_out.at[c], x_in.at[c], x_send.at[c], x_recv.at[c], ep=partner)

    def home(c):
        return remote(
            r_out.at[c], r_in.at[c], r_send.at[c], r_recv.at[c], ep=2 * chip(c) + core
        )

    def home_square(c, k):
        return remote(
            so_out.at[c], so_in.at[c, k], so_send.at[c, k], so_recv.at[c, k],
            ep=2 * chip(c) + core, tp=(x_tp, y_tp, xy_tp, tp)[k],
        )

    def take_in(c):
        dispatch(c).wait_recv()
        forward(c, core).start()

    waited = set()

    def arrive(copy, *which):
        if (copy, which) not in waited:
            waited.add((copy, which))
            copy(*which).wait_recv()

    def gate_up(c, p):
        if p == 0:
            forward(c, other).wait_recv()
            raw = compact[c].reshape(2 * rows_z, width).astype(F32)
            square = jnp.sum(raw * raw, axis=1, keepdims=True)
            diag = iota((2 * rows_z, 128), 0) == iota((2 * rows_z, 128), 1)
            row = jnp.sum(jnp.where(diag, square, 0.0), axis=0, keepdims=True)
            ss_out[c] = jnp.broadcast_to(row, (8, 128))
            for k in range(3):
                square_copy(c, k).start()
            gained = (raw * in_gain_ref[...]).astype(BF16)
            rows[c] = (
                jnp.dot(pick[c].reshape(n_slot, 2 * rows_z), gained, preferred_element_type=F32)
                .astype(BF16)
            )
        e = expert(p)
        if c == 0:
            w_copy(0, p).wait()
            w_copy(1, p).wait()
        for h in range(2):
            cols = slice(h * half, (h + 1) * half)
            part[c, h, p, :, 0:half] = jnp.dot(
                rows[c], wg[e, :, cols], preferred_element_type=F32
            ).astype(BF16)
            part[c, h, p, :, half:ff] = jnp.dot(
                rows[c], wu[e, :, cols], preferred_element_type=F32
            ).astype(BF16)
        if p < 2:
            s1(c, 0, p, p).start()
        if p % 2 == 0:
            s1(c, 1, p // 2, p).start()

    def reduce_first(c, h):
        s1(c, h, 0, 0).wait_recv()
        s2_out[c, h] = (mine(c, h, 2 - h)[...].astype(F32) + s1_in[c, h, 0].astype(F32)).astype(BF16)
        s2(c, h).start()

    def activate(c, h):
        for k in range(3):
            arrive(square_copy, c, k)
        square = ss_out[c] + ss_in[c, 0] + ss_in[c, 1] + ss_in[c, 2]
        scale_row = lax.rsqrt(square[0:1, 0 : 2 * rows_z] / D + EPS)
        scale = jnp.sum(pick[c, tp].astype(F32) * scale_row, axis=1, keepdims=True)
        weight = slot_w[c, tp][:, 0:1]
        s1(c, h, 1, 3).wait_recv()
        s2(c, h).wait_recv()
        total = (
            mine(c, h, 3)[...].astype(F32) + s1_in[c, h, 1].astype(F32) + s2_in[c, h].astype(F32)
        ) * scale
        gate, up = total[:, 0:half], total[:, half:ff]
        act[c, h, tp] = (gate / (1.0 + jnp.exp(-gate)) * up * weight).astype(BF16)
        gather(c, h, h).start()
        if h == 1:
            gather(c, 1, 0).start()
            gather(c, 0, 1).start()

    def pass_on(c, h):
        arrive(gather, c, h, h)
        relay(c, h).start()

    def down(c, i):
        p = (3, 1, 2, 0)[i]
        e = expert(p)
        for h in range(2):
            if i == n_exp - 1:
                relay(c, h).wait_recv()
            elif i:
                arrive(gather, c, h, i - 1)
        if ("down", p) not in waited:
            waited.add(("down", p))
            w_copy(2, p).wait()
        wide[...] = (
            jnp.dot(jnp.concatenate([act[c, 0, e]] * 4), wd[e, 0:half], preferred_element_type=F32)
            + jnp.dot(jnp.concatenate([act[c, 1, e]] * 4), wd[e, half:], preferred_element_type=F32)
        ).astype(BF16)
        res[c, e] = wide[0:slots]
        if i == n_exp - 1:
            comb[c] = tdot(
                pick[c].reshape(n_slot, 2 * rows_z), res[c].reshape(n_slot, width)
            ).reshape(2, rows_z, width)
            x_out[c] = comb[c, other].astype(BF16)
            swap(c).start()

    def send_home(c):
        swap(c).wait_recv()
        total = comb[c, core] + x_in[c].astype(F32)
        square = jnp.sum(total * total, axis=1, keepdims=True)
        diag = c * rows_z + iota((rows_z, 128), 0) == iota((rows_z, 128), 1)
        row = jnp.sum(jnp.where(diag, square, 0.0), axis=0, keepdims=True)
        so_out[c] = jnp.broadcast_to(row, (8, 128))
        for k in range(4 if c else 3):
            home_square(c, k).start()
        if c:
            r_out[c] = total.astype(BF16)
            home(c).start()
        else:
            r_in[0] = total.astype(BF16)
            so_in[0, 3] = so_out[0]

    stage = {
        "A": gate_up,
        "B": reduce_first,
        "C": activate,
        "D": pass_on,
        "E": down,
        "F": send_home,
        "N": take_in,
        "P": make_pick,
    }
    for step in ORDER:
        with jax.named_scope(step):
            stage[step[0]](*(int(digit) for digit in step[1:]))

    for c in range(n_z):
        forward(c, core).wait_send()
        if c:
            dispatch(c).wait_send()
        for k in range(3):
            square_copy(c, k).wait_send()
        for h in range(2):
            s1(c, h, 0, 0).wait_send()
            s1(c, h, 1, 1 + h).wait_send()
            s2(c, h).wait_send()
            gather(c, h, 0).wait_send()
            gather(c, h, 1).wait_send()
            relay(c, h).wait_send()
        swap(c).wait_send()

    for c in range(1, n_z):
        home(c).wait_recv()
    combined[...] = jnp.dot(
        own_pick[...], r_in[...].reshape(n_z * rows_z, width), preferred_element_type=F32
    )
    square = so_in[0, 3]
    for c in range(n_z):
        for k in range(4 if c else 3):
            home_square(c, k).wait_recv()
            square = square + so_in[c, k]
    scale_row = lax.rsqrt(square[0:1, :] / D + EPS)
    scale = jnp.sum(own_pick[...].astype(F32) * scale_row, axis=1, keepdims=True)
    out_ref[...] = (combined[...] * scale * out_gain_ref[...]).astype(BF16)

    for c in range(n_z):
        if c:
            home(c).wait_send()
        for k in range(4 if c else 3):
            home_square(c, k).wait_send()


def fused(mesh, tokens, in_gain, out_gain, routes, route_weights, w_gate, w_up, w_down):
    tok, width = tokens.shape
    top = routes.shape[1]
    n_exp, _, ff = w_gate.shape
    n_ep = mesh.shape["ep"]
    n_z = n_ep // 2
    cap = max(2, 2 * tok * top // (n_exp * n_ep))
    rows_z = cap * GROUP // top
    slots = 2 * cap
    cfg = (n_z, tok, n_exp, cap, width, ff, top)
    vmem = pl.BlockSpec(memory_space=pltpu.VMEM)
    hbm = pl.BlockSpec(memory_space=pl.ANY)
    dma = pltpu.SemaphoreType.DMA
    return pl.pallas_call(
        functools.partial(kernel, cfg),
        out_shape=jax.ShapeDtypeStruct((tok, width), BF16),
        in_specs=[hbm] * 8,
        out_specs=vmem,
        scratch_shapes=[
            pltpu.VMEM((tok, width), BF16),
            pltpu.VMEM((1, width), F32),
            pltpu.VMEM((1, width), F32),
            pltpu.VMEM((top, n_ep * tok), jnp.int32),
            pltpu.VMEM((top, n_ep * tok), F32),
            pltpu.VMEM(w_gate.shape, BF16),
            pltpu.VMEM(w_up.shape, BF16),
            pltpu.VMEM(w_down.shape, BF16),
            pltpu.VMEM((n_z, n_exp, slots, 2 * rows_z), BF16),
            pltpu.VMEM((n_z, n_exp, slots, 128), F32),
            pltpu.VMEM((tok, n_z * rows_z), BF16),
            pltpu.VMEM((n_z, rows_z, width), BF16),
            pltpu.VMEM((n_z, 2, rows_z, width), BF16),
            pltpu.VMEM((n_z, n_exp * slots, width), BF16),
            pltpu.VMEM((n_z, 8, 128), F32),
            pltpu.VMEM((n_z, 3, 8, 128), F32),
            pltpu.VMEM((n_z, 2, n_exp, n_exp * slots, ff), BF16),
            pltpu.VMEM((n_z, 2, 2, slots, ff), BF16),
            pltpu.VMEM((n_z, 2, slots, ff), BF16),
            pltpu.VMEM((n_z, 2, slots, ff), BF16),
            pltpu.VMEM((n_z, 2, n_exp, slots, ff // 2), BF16),
            pltpu.VMEM((n_z, n_exp, slots, width), BF16),
            pltpu.VMEM((4 * slots, width), BF16),
            pltpu.VMEM((n_z, 2, rows_z, width), F32),
            pltpu.VMEM((tok, width), F32),
            pltpu.VMEM((n_z, rows_z, width), BF16),
            pltpu.VMEM((n_z, rows_z, width), BF16),
            pltpu.VMEM((n_z, rows_z, width), BF16),
            pltpu.VMEM((n_z, rows_z, width), BF16),
            pltpu.VMEM((n_z, 8, 128), F32),
            pltpu.VMEM((n_z, 4, 8, 128), F32),
            dma((5,)),
            dma((3, n_exp)),
            dma((n_z,)),
            dma((n_z, 2)),
            dma((n_z,)),
            dma((n_z, 3)),
            dma((n_z, 3)),
            dma((n_z, 2, 2)),
            dma((n_z, 2, 2)),
            dma((n_z, 2)),
            dma((n_z, 2)),
            dma((n_z, 2, 3)),
            dma((n_z, 2, 3)),
            dma((n_z,)),
            dma((n_z,)),
            dma((n_z,)),
            dma((n_z,)),
            dma((n_z, 4)),
            dma((n_z, 4)),
        ],
        compiler_params=pltpu.CompilerParams(
            collective_id=0, has_side_effects=True, vmem_limit_bytes=52 * 2**20
        ),
    )(
        *(
            pltpu.with_memory_space_constraint(array, pltpu.HBM)
            for array in (
                tokens,
                in_gain.reshape(1, width),
                out_gain.reshape(1, width),
                routes.T,
                route_weights.T,
                w_gate,
                w_up,
                w_down,
            )
        )
    )


def run_experts(slot_rows, w_gate, w_up, w_down):
    gate_part = jnp.einsum(
        "secd,edf->secf", slot_rows, w_gate, preferred_element_type=jnp.float32
    ).astype(jnp.bfloat16)
    up_part = jnp.einsum(
        "secd,edf->secf", slot_rows, w_up, preferred_element_type=jnp.float32
    ).astype(jnp.bfloat16)
    gate_sum, up_sum = (
        lax.psum(gate_part, "tp").astype(jnp.float32),
        lax.psum(up_part, "tp").astype(jnp.float32),
    )
    active = (jax.nn.silu(gate_sum) * up_sum).astype(jnp.bfloat16)
    return jnp.einsum("secf,efd->secd", active, w_down, preferred_element_type=jnp.float32).astype(
        jnp.bfloat16
    )


def on_device(tokens, in_gain, out_gain, routes, route_weights, w_gate, w_up, w_down):
    tok_rows, local_width = tokens.shape
    top_count = routes.shape[1]
    local_experts = w_gate.shape[0]
    groups_ep = lax.axis_size("ep")
    experts = local_experts * groups_ep
    capacity = max(2, 2 * tok_rows * top_count // experts)
    values = tokens.astype(jnp.float32)
    sum_squares = lax.psum(jnp.sum(values * values, axis=1), "tp")
    normed = (values * lax.rsqrt(sum_squares / D + EPS)[:, None] * in_gain).astype(jnp.bfloat16)
    row_start = lax.axis_index("ep") * tok_rows
    my_routes = lax.dynamic_slice_in_dim(routes, row_start, tok_rows, 0)
    my_weights = lax.dynamic_slice_in_dim(route_weights, row_start, tok_rows, 0)
    flat_ids = my_routes.reshape(-1)
    matches = (flat_ids[:, None] == jnp.arange(experts, dtype=jnp.int32)[None, :]).astype(jnp.int32)
    slot_rank = jnp.sum((jnp.cumsum(matches, axis=0) - matches) * matches, axis=1)
    position = flat_ids * capacity + slot_rank
    dispatch_table = jnp.any(
        position.reshape(tok_rows, top_count, 1)
        == jnp.arange(experts * capacity, dtype=jnp.int32)[None, None, :],
        axis=1,
    )
    outgoing = jnp.einsum(
        "ts,td->sd", dispatch_table.astype(jnp.bfloat16), normed, preferred_element_type=jnp.float32
    ).astype(jnp.bfloat16)
    outgoing = outgoing.reshape(groups_ep, local_experts, capacity, local_width)
    answers = run_experts(
        lax.all_to_all(outgoing, "ep", split_axis=0, concat_axis=0, tiled=True),
        w_gate,
        w_up,
        w_down,
    )
    returned = lax.all_to_all(answers, "ep", split_axis=0, concat_axis=0, tiled=True)
    flat_out = returned.reshape(experts * capacity, local_width)
    picked = flat_out[position].reshape(tok_rows, top_count, local_width)
    combined = jnp.sum(my_weights[:, :, None] * picked.astype(jnp.float32), axis=1)
    out_squares = lax.psum(jnp.sum(combined * combined, axis=1), "tp")
    return (combined * lax.rsqrt(out_squares / D + EPS)[:, None] * out_gain).astype(jnp.bfloat16)


def solution(mesh):
    placed = (
        P("ep", "tp"),
        P("tp"),
        P("tp"),
        P(),
        P(),
        P("ep", "tp", None),
        P("ep", "tp", None),
        P("ep", None, "tp"),
    )
    body = on_device
    if mesh.shape["tp"] == 4 and mesh.shape["ep"] == 8:
        body = functools.partial(fused, mesh)
    return jax.shard_map(
        body, mesh=mesh, in_specs=placed, out_specs=P("ep", "tp"), check_vma=False
    )
```
